32 devices in a mesh: sp: 4 (over y, x), tp: 8 (over z, core).
Axes of the slice: x: 2, y: 2, z: 4, core: 2. Of those that a mesh axis runs over, the one named last changes fastest.
Arguments:
- target: bfloat16 [512, 2048], P('sp'), may hold values from -6 to 6
- source: bfloat16 [1536, 2048], P('sp'), may hold values from -6 to 6
- cotangent: bfloat16 [512, 2048], P('sp'), may hold values from -192 to 192
- target_gain: float32 [2048], replicated, may hold values from 0.1 to 1.9
- source_gain: float32 [2048], replicated, may hold values from 0.1 to 1.9
- w_query: bfloat16 [2048, 4096], P(None, 'tp'), may hold values from -0.125 to 0.125
- w_key: bfloat16 [2048, 128], replicated, may hold values from -0.125 to 0.125
- w_value: bfloat16 [2048, 128], replicated, may hold values from -0.125 to 0.125
- w_out: bfloat16 [4096, 2048], P('tp'), may hold values from -0.09375 to 0.09375
Outputs:
- grad_target: bfloat16 [512, 2048], P(('sp', 'tp'))
- grad_source: bfloat16 [1536, 2048], P(('sp', 'tp'))
- grad_out_w: bfloat16 [4096, 2048], P('tp', 'sp')
The draws below stay inside these ranges and needn't reach their ends.
All inputs are finite; a program needn't handle non-finite values.
Results may differ from the reference program's by a relative error of at most 0.025.
Values may be sent and summed in bfloat16 or wider, within the bound.
A program may use at most 64 MiB of HBM per device.

```python
import jax
import jax.numpy as jnp
from jax import lax

D = 2048
HEADS = 32
HEAD = 128
TARGET = 512
SOURCE = 1536


def steps_of(own_key, dims, shards, low, largest):
    level = 1.0
    for dim, shards_of in shards:
        draws = jax.random.uniform(jax.random.fold_in(jax.random.fold_in(own_key, 6), dim), (shards_of,), jnp.float32, low / len(shards), largest / len(shards))
        level = level * jnp.repeat(jnp.exp(draws), dims[dim] // shards_of).reshape((-1,) + (1,) * (len(dims) - 1 - dim))
    return level


def bell_draw(own_key, extent, spread, bound, split=(), kind=jnp.bfloat16):
    result = spread * jax.random.normal(own_key, extent, jnp.float32)
    if split:
        result = result * steps_of(own_key, extent, split, -0.22, 0.18)
    return jnp.clip(result, -bound, bound).astype(kind)


def setup_inputs(seed: int = 0) -> dict:
    key_of = jax.random.split(jax.random.key(seed), 10)
    return {
        "target": bell_draw(key_of[0], (TARGET, D), 1.0, 6.0, ((0, 4),)),
        "source": bell_draw(key_of[1], (SOURCE, D), 1.0, 6.0, ((0, 4),)),
        "cotangent": bell_draw(key_of[2], (TARGET, D), 32.0, 192.0, ((0, 4),)),
        "target_gain": jnp.clip(1.0 + 0.18 * jax.random.normal(key_of[3], (D,), jnp.float32), 0.1, 1.9),
        "source_gain": jnp.clip(1.0 + 0.18 * jax.random.normal(key_of[4], (D,), jnp.float32), 0.1, 1.9),
        "w_query": bell_draw(key_of[5], (D, HEADS * HEAD), D ** -0.5, 0.125, ((1, 8),)),
        "w_key": bell_draw(key_of[6], (D, HEAD), D ** -0.5, 0.125),
        "w_value": bell_draw(key_of[7], (D, HEAD), D ** -0.5, 0.125),
        "w_out": bell_draw(key_of[8], (HEADS * HEAD, D), (HEADS * HEAD) ** -0.5, 0.09375, ((0, 8),)),
    }


NORM_EPS = 1e-06

def normed(row_block, gain_vec):
    rows_wide = row_block.astype(jnp.float32)
    inv_rms = lax.rsqrt(lax.optimization_barrier(jnp.mean(rows_wide * rows_wide, axis=1, keepdims=True)) + NORM_EPS)
    return (rows_wide * inv_rms * gain_vec).astype(jnp.bfloat16)

def norm_back(row_block, gain_vec, upstream):
    rows_wide = row_block.astype(jnp.float32)
    inv_rms = lax.rsqrt(lax.optimization_barrier(jnp.mean(rows_wide * rows_wide, axis=1, keepdims=True)) + NORM_EPS)
    unit_rows = rows_wide * inv_rms
    pulled = upstream * gain_vec
    return inv_rms * (pulled - unit_rows * lax.optimization_barrier(jnp.mean(pulled * unit_rows, axis=1, keepdims=True)))

def reference(target, source, cotangent, target_gain, source_gain, w_query, w_key, w_value, w_out):
    inv_root = HEAD ** (-0.5)
    normed_target = normed(target, target_gain)
    query_rows = jnp.dot(normed_target, w_query, preferred_element_type=jnp.float32).astype(jnp.bfloat16)
    normed_source = normed(source, source_gain)
    key_rows = jnp.dot(normed_source, w_key, preferred_element_type=jnp.float32).astype(jnp.bfloat16)
    value_rows = jnp.dot(normed_source, w_value, preferred_element_type=jnp.float32).astype(jnp.bfloat16)
    grad_attn = jnp.dot(cotangent, w_out.T, preferred_element_type=jnp.float32).astype(jnp.bfloat16)
    query_heads = query_rows.reshape(TARGET, HEADS, HEAD).transpose(1, 0, 2)
    grad_heads = grad_attn.reshape(TARGET, HEADS, HEAD).transpose(1, 0, 2)

    def one_head(carried, head_pair):
        key_sum, value_sum = carried
        query_one, grad_one = head_pair
        scores = jnp.dot(query_one, key_rows.T, preferred_element_type=jnp.float32) * inv_root
        exponent = jnp.exp(scores)
        row_total = lax.optimization_barrier(jnp.sum(exponent, axis=1))
        weights = exponent.astype(jnp.bfloat16)
        attended = (jnp.dot(weights, value_rows, preferred_element_type=jnp.float32) / row_total[:, None]).astype(jnp.bfloat16)
        prob_grad = jnp.dot(grad_one, value_rows.T, preferred_element_type=jnp.float32)
        delta_row = lax.optimization_barrier(jnp.sum(attended.astype(jnp.float32) * grad_one.astype(jnp.float32), axis=1))
        tilted = (exponent * prob_grad).astype(jnp.bfloat16)
        tilted_sum = jnp.dot(tilted, key_rows, preferred_element_type=jnp.float32)
        weight_sum = jnp.dot(weights, key_rows, preferred_element_type=jnp.float32)
        grad_query = ((tilted_sum - delta_row[:, None] * weight_sum) / row_total[:, None] * inv_root).astype(jnp.bfloat16)
        prob_rows = exponent / row_total[:, None]
        score_grad = (prob_rows * (prob_grad - delta_row[:, None])).astype(jnp.bfloat16)
        key_grad = jnp.dot(score_grad.T, query_one, preferred_element_type=jnp.float32) * inv_root
        value_grad = jnp.dot(prob_rows.astype(jnp.bfloat16).T, grad_one, preferred_element_type=jnp.float32)
        return ((key_sum + key_grad, value_sum + value_grad), (attended, grad_query))
    empty_keys = jnp.zeros((SOURCE, HEAD), jnp.float32)
    sums, stacked = lax.scan(one_head, (empty_keys, empty_keys), (query_heads, grad_heads))
    key_grad, value_grad = sums
    attended_heads, query_grad_heads = stacked
    attended_rows = attended_heads.transpose(1, 0, 2).reshape(TARGET, HEADS * HEAD)
    query_grad_rows = query_grad_heads.transpose(1, 0, 2).reshape(TARGET, HEADS * HEAD)
    pulled_source = jnp.dot(key_grad.astype(jnp.bfloat16), w_key.T, preferred_element_type=jnp.float32)
    pulled_source = pulled_source + jnp.dot(value_grad.astype(jnp.bfloat16), w_value.T, preferred_element_type=jnp.float32)
    grad_source = norm_back(source, source_gain, pulled_source).astype(jnp.bfloat16)
    pulled_target = jnp.dot(query_grad_rows, w_query.T, preferred_element_type=jnp.float32)
    grad_target = norm_back(target, target_gain, pulled_target).astype(jnp.bfloat16)
    grad_out_w = jnp.dot(attended_rows.T, cotangent, preferred_element_type=jnp.float32).astype(jnp.bfloat16)
    return (grad_target, grad_source, grad_out_w)
```

```python
import functools
import math

import jax
import jax.numpy as jnp
from jax import lax
from jax.experimental import pallas as pl
from jax.experimental.pallas import tpu as pltpu
from jax.sharding import PartitionSpec as P

HEAD = 128
NORM_EPS = 1e-06
CORES = 2
F32 = jnp.float32
BF16 = jnp.bfloat16
MESH = pl.DeviceIdType.MESH
NN = (((1,), (0,)), ((), ()))
NT = (((1,), (1,)), ((), ()))
TN = (((0,), (0,)), ((), ()))


def dot(a, b, dims=NN):
    return lax.dot_general(a, b, dims, preferred_element_type=F32)


def inv_rms_of(wide):
    return lax.rsqrt(jnp.mean(wide * wide, axis=1, keepdims=True) + NORM_EPS)


def norm_into(src, gain, dst, block):
    def body(i, _):
        rows = pl.ds(pl.multiple_of(i * block, block), block)
        wide = src[rows, :].astype(F32)
        dst[rows, :] = (wide * inv_rms_of(wide) * gain[...]).astype(BF16)
        return 0

    lax.fori_loop(0, src.shape[0] // block, body, 0)


def norm_back(wide, gain, upstream):
    inv = inv_rms_of(wide)
    unit = wide * inv
    pulled = upstream * gain
    return inv * (pulled - unit * jnp.mean(pulled * unit, axis=1, keepdims=True))


def own_rows(ref, place, rows):
    if rows % 16 == 0:
        return ref[pl.ds(pl.multiple_of(place * rows, 16), rows), :].astype(F32)
    padded = -(-rows // 16) * 16
    line = lax.broadcasted_iota(jnp.int32, (padded, ref.shape[0]), 0) + place * rows
    column = lax.broadcasted_iota(jnp.int32, (padded, ref.shape[0]), 1)
    pick = jnp.where(line == column, 1.0, 0.0).astype(BF16)
    return dot(pick, ref[...])[:rows]


def kernel(
    S, T,
    target_h, source_h, cot_h, tgain, sgain, wq_h, wk_h, wv_h, wo_h,
    gt_ref, gs_ref, go_ref,
    target, source, cot, wq, wkv, wo, normed, kv, cotb, att, e_buf,
    kvg, kvg_in, red, red_in, red2, fin_in, pt, pt_in, ptr, ptr_in, stage,
    load_sem, send, recv,
):
    Z = T // CORES
    me, t = lax.axis_index("sp"), lax.axis_index("tp")
    c, z = lax.rem(t, CORES), lax.div(t, CORES)
    sibling = {"sp": me, "tp": z * CORES + (1 - c)}
    TR, D = target.shape
    SG = source.shape[0]
    QW = wq.shape[1]
    H = QW // HEAD
    half = SG // 2
    thalf = TR // 2
    W = D // S
    SR, RR = SG // T, TR // T
    inv_root = HEAD ** (-0.5)

    def sp_peer(d):
        return {"sp": lax.rem(me + d, S), "tp": t}

    def z_peer(d):
        return {"sp": me, "tp": lax.rem(z + d, Z) * CORES + c}

    sends = []

    def put(src, dst, lane, slot, who):
        copy = pltpu.make_async_remote_copy(
            src_ref=src, dst_ref=dst, send_sem=send.at[lane, slot], recv_sem=recv.at[lane, slot],
            device_id=who, device_id_type=MESH,
        )
        copy.start()
        sends.append(copy)
        return copy

    loads = []
    for i, (a, b) in enumerate(
        (
            (source_h, source), (wk_h, wkv.at[:, :HEAD]), (wv_h, wkv.at[:, HEAD:]),
            (target_h, target), (wq_h, wq), (cot_h, cot), (wo_h, wo),
        )
    ):
        copy = pltpu.make_async_copy(a, b, load_sem.at[i])
        copy.start()
        loads.append(copy)

    barrier = pltpu.get_barrier_semaphore()
    friends = [sibling] + [sp_peer(d) for d in range(1, S)] + [z_peer(d) for d in range(1, Z)]
    for who in friends:
        pl.semaphore_signal(barrier, inc=1, device_id=who, device_id_type=MESH)

    loads[0].wait()
    norm_into(source, sgain, normed, 32)
    loads[1].wait()
    loads[2].wait()
    kv_own = dot(normed[...], wkv[...]).astype(BF16)
    kv[0, 0] = kv_own[:half]
    kv[0, 1] = kv_own[half:]
    pl.semaphore_wait(barrier, len(friends))
    kv_put = [None] + [put(kv.at[0, c], kv.at[d, c], 0, d, sp_peer(d)) for d in range(1, S)]
    loads[5].wait()
    cot_put = [None]
    for d in range(1, S):
        columns = pl.ds(pl.multiple_of(lax.rem(me + d, S) * W, 128), W)
        rows = pl.ds(pl.multiple_of(c * thalf, thalf), thalf)
        cot_put.append(put(cot.at[rows, columns], cotb.at[d, c], 1, d, sp_peer(d)))

    loads[3].wait()
    norm_into(target, tgain, normed, 32)
    loads[4].wait()
    query = dot(normed[:TR, :], wq[...]).astype(BF16)
    loads[6].wait()
    grad = dot(cot[...], wo[...], NT).astype(BF16)
    q_rows = jnp.concatenate([query[:, h * HEAD:(h + 1) * HEAD] for h in range(H)], axis=0)
    g_rows = jnp.concatenate([grad[:, h * HEAD:(h + 1) * HEAD] for h in range(H)], axis=0)

    def pair(d):
        both = jnp.concatenate([kv[d,0],kv[d,1]],axis=0)
        return both[:, :HEAD], both[:, HEAD:]

    def exponents(d):
        k, v = pair(d)
        e = jnp.exp2(dot(k, q_rows, NT) * (inv_root * math.log2(math.e)))
        e_buf[d] = e
        return jnp.sum(e, axis=0, keepdims=True), dot(v, e.astype(BF16), TN)

    total, out_t = exponents(0)
    kv_fwd = [None]
    for d in range(1, S):
        kv_put[d].wait_recv()
        kv_fwd.append(put(kv.at[d, c], kv.at[d, c], 2, d, sibling))
    for d in range(1, S):
        kv_fwd[d].wait_recv()
        more, out_more = exponents(d)
        total, out_t = total + more, out_t + out_more
    inv_total = 1.0 / total
    att_t = (out_t * inv_total).astype(BF16)
    att[0] = att_t
    delta = jnp.sum(att_t.astype(F32) * g_rows.astype(F32).T, axis=0, keepdims=True)
    att_put = [None] + [put(att.at[0], att.at[d], 3, d, sp_peer(d)) for d in range(1, S)]

    def spread(d, grads):
        if SR % 8:
            stage[...] = grads
        for place in range(T):
            rows = slice(place * SR, (place + 1) * SR)
            block = stage[rows, :] if SR % 8 else grads[rows]
            kvg[place % CORES, d, place // CORES] = block.astype(BF16)

    def settle(d):
        kvg_put[d].wait_recv()
        red[d] = (kvg[c, d].astype(F32) + kvg_in[d].astype(F32)).astype(BF16)
        if d:
            return put(red.at[d], red_in.at[d], 5, d, sp_peer(S - d))

    kvg_put = {}
    red_put = {}
    gq_t = None
    order = list(range(1, S)) + [0]
    for step, d in enumerate(order):
        k, v = pair(d)
        p = e_buf[d] * inv_total
        score_grad = (p * (dot(v, g_rows, NT) - delta)).astype(BF16)
        part = dot(k, score_grad, TN)
        gq_t = part if gq_t is None else gq_t + part
        k_grad = dot(score_grad, q_rows) * inv_root
        v_grad = dot(p.astype(BF16), g_rows)
        spread(d, jnp.concatenate([k_grad, v_grad], axis=1))
        kvg_put[d] = put(kvg.at[1 - c, d], kvg_in.at[d], 4, d, sibling)
        if step:
            red_put[order[step - 1]] = settle(order[step - 1])

    gq_t = gq_t * inv_root
    gq = jnp.concatenate([gq_t[:, h * TR:(h + 1) * TR].T for h in range(H)], axis=1).astype(BF16)
    pulled = dot(gq, wq[...], NT)
    for place in range(T):
        if RR % 8:
            if place == 0:
                normed_rows = stage_rows(e_buf, pulled)
            block = normed_rows(place * RR, RR)
        else:
            block = pulled[place * RR:(place + 1) * RR]
        pt[place % CORES, place // CORES] = block.astype(BF16)
    pt_put = put(pt.at[1 - c], pt_in, 6, 0, sibling)
    settle(0)
    cot_fwd = [None]
    for d in range(1, S):
        cot_put[d].wait_recv()
        cot_fwd.append(put(cotb.at[d, c], cotb.at[d, c], 7, d, sibling))
    pt_put.wait_recv()
    ptr[...] = (pt[c].astype(F32) + pt_in[...].astype(F32)).astype(BF16)
    ptr_put = [None] + [
        put(ptr.at[lax.rem(z + d, Z)], ptr_in.at[d], 8, d, z_peer(d)) for d in range(1, Z)
    ]
    summed = red[0].astype(F32)
    for d in range(1, S):
        red_put[d].wait_recv()
        summed = summed + red_in[d].astype(F32)
    red2[...] = summed.astype(BF16)
    fin_put = [None] + [
        put(red2.at[lax.rem(z + d, Z)], fin_in.at[d], 9, d, z_peer(d)) for d in range(1, Z)
    ]

    att_all, cot_all = [att[0]], [cot[:, pl.ds(pl.multiple_of(me * W, 128), W)]]
    for d in range(1, S):
        att_put[d].wait_recv()
        cot_fwd[d].wait_recv()
        att_all.append(att[d])
        cot_all.append(jnp.concatenate([cotb[d,0],cotb[d,1]],axis=0))
    cot_rows = jnp.concatenate(cot_all, axis=0)
    for h in range(H):
        left = jnp.concatenate([a[:, h * TR:(h + 1) * TR] for a in att_all], axis=1)
        go_ref[h * HEAD:(h + 1) * HEAD, :] = dot(left, cot_rows).astype(BF16)

    up = ptr[z].astype(F32)
    for d in range(1, Z):
        ptr_put[d].wait_recv()
        up = up + ptr_in[d].astype(F32)
    gt_ref[...] = norm_back(own_rows(target, t, RR), tgain[...], up).astype(BF16)
    last = red2[z].astype(F32)
    for d in range(1, Z):
        fin_put[d].wait_recv()
        last = last + fin_in[d].astype(F32)
    up = dot(last.astype(BF16), wkv[...], NT)
    gs_ref[...] = norm_back(own_rows(source, t, SR), sgain[...], up).astype(BF16)
    for copy in sends:
        copy.wait_send()


def stage_rows(buf, rows):
    width = buf.shape[2]
    bands = rows.shape[1] // width
    for i in range(bands):
        buf[i, :rows.shape[0], :] = rows[:, i * width:(i + 1) * width]
    return lambda start, count: jnp.concatenate(
        [buf[i, start:start + count, :] for i in range(bands)], axis=1
    )


def on_device(S, T, target, source, cotangent, target_gain, source_gain, w_query, w_key, w_value, w_out):
    TR, D = target.shape
    SG = source.shape[0]
    QW = w_query.shape[1]
    R = QW // HEAD * TR
    Z = T // CORES
    SR, RR, W = SG // T, TR // T, D // S
    N = max(S, Z)
    hbm = pl.BlockSpec(memory_space=pl.ANY)
    vm = pl.BlockSpec(memory_space=pltpu.VMEM)
    V = pltpu.VMEM
    return pl.pallas_call(
        functools.partial(kernel, S, T),
        out_shape=(
            jax.ShapeDtypeStruct((RR, D), BF16),
            jax.ShapeDtypeStruct((SR, D), BF16),
            jax.ShapeDtypeStruct((QW, W), BF16),
        ),
        in_specs=[hbm, hbm, hbm, vm, vm, hbm, hbm, hbm, hbm],
        out_specs=(vm, vm, vm),
        scratch_shapes=[
            V((TR, D), BF16), V((SG, D), BF16), V((TR, D), BF16),
            V((D, QW), BF16), V((D, 2 * HEAD), BF16), V((QW, D), BF16),
            V((max(SG, TR), D), BF16),
            V((S, 2, SG // 2, 2 * HEAD), BF16), V((S, 2, TR // 2, W), BF16),
            V((S, HEAD, R), BF16), V((S, SG, R), F32),
            V((CORES, S, Z, SR, 2 * HEAD), BF16), V((S, Z, SR, 2 * HEAD), BF16),
            V((S, Z, SR, 2 * HEAD), BF16), V((S, Z, SR, 2 * HEAD), BF16),
            V((Z, SR, 2 * HEAD), BF16), V((Z, SR, 2 * HEAD), BF16),
            V((CORES, Z, RR, D), BF16), V((Z, RR, D), BF16), V((Z, RR, D), BF16), V((Z, RR, D), BF16),
            V((SG, 2 * HEAD), F32),
            pltpu.SemaphoreType.DMA((7,)),
            pltpu.SemaphoreType.DMA((10, N)),
            pltpu.SemaphoreType.DMA((10, N)),
        ],
        compiler_params=pltpu.CompilerParams(
            collective_id=0, has_side_effects=True, vmem_limit_bytes=60 * 1024 * 1024
        ),
        name="attn_back",
    )(
        target, source, cotangent, target_gain.reshape(1, D), source_gain.reshape(1, D),
        w_query, w_key, w_value, w_out,
    )


def solution(mesh):
    in_specs = (
        P("sp", None), P("sp", None), P("sp", None), P(), P(),
        P(None, "tp"), P(), P(), P("tp", None),
    )
    out_specs = (P(("sp", "tp"), None), P(("sp", "tp"), None), P("tp", "sp"))
    return jax.shard_map(
        functools.partial(on_device, mesh.shape["sp"], mesh.shape["tp"]),
        mesh=mesh, in_specs=in_specs, out_specs=out_specs, check_vma=False,
    )
```

```python
import functools
import math

import jax
import jax.numpy as jnp
from jax import lax
from jax.experimental import pallas as pl
from jax.experimental.pallas import tpu as pltpu
from jax.sharding import PartitionSpec as P

HEAD = 128
NORM_EPS = 1e-06
CORES = 2
F32 = jnp.float32
BF16 = jnp.bfloat16
MESH = pl.DeviceIdType.MESH
NN = (((1,), (0,)), ((), ()))
NT = (((1,), (1,)), ((), ()))
TN = (((0,), (0,)), ((), ()))


def dot(a, b, dims=NN):
    return lax.dot_general(a, b, dims, preferred_element_type=F32)


def inv_rms_of(wide):
    return lax.rsqrt(jnp.mean(wide * wide, axis=1, keepdims=True) + NORM_EPS)


def norm_into(src, gain, dst, block, base, count):
    def body(i, _):
        rows = pl.ds(pl.multiple_of(base + i * block, block), block)
        wide = src[rows, :].astype(F32)
        dst[rows, :] = (wide * inv_rms_of(wide) * gain[...]).astype(BF16)
        return 0

    lax.fori_loop(0, count // block, body, 0)


def norm_back(wide, gain, upstream):
    inv = inv_rms_of(wide)
    unit = wide * inv
    pulled = upstream * gain
    return inv * (pulled - unit * jnp.mean(pulled * unit, axis=1, keepdims=True))


def own_rows(ref, place, rows):
    if rows % 16 == 0:
        return ref[pl.ds(pl.multiple_of(place * rows, 16), rows), :].astype(F32)
    padded = -(-rows // 16) * 16
    line = lax.broadcasted_iota(jnp.int32, (padded, ref.shape[0]), 0) + place * rows
    column = lax.broadcasted_iota(jnp.int32, (padded, ref.shape[0]), 1)
    pick = jnp.where(line == column, 1.0, 0.0).astype(BF16)
    return dot(pick, ref[...])[:rows]


def kernel(
    S, T,
    target_h, source_h, cot_h, tgain_h, sgain_h, wq_h, wk_h, wv_h, wo_h,
    gt_out, gs_out, go_out,
    target, source, cot, tgain, sgain, wq, wkv, wo, normed, kv, cotb, att, e_buf,
    kvg, kvg_in, red, red_in, red2, fin_in, pt, pt_in, ptr, ptr_in, stage,
    gt_ref, gs_ref, go_ref, load_sem, send, recv,
):
    Z = T // CORES
    me, t = lax.axis_index("sp"), lax.axis_index("tp")
    c, z = lax.rem(t, CORES), lax.div(t, CORES)
    sibling = {"sp": me, "tp": z * CORES + (1 - c)}
    TR, D = target.shape
    SG = source.shape[0]
    QW = wq.shape[1]
    H = QW // HEAD
    half = SG // 2
    thalf = TR // 2
    W = D // S
    SR, RR = SG // T, TR // T
    inv_root = HEAD ** (-0.5)

    X = math.isqrt(S) if math.isqrt(S) ** 2 == S else S
    Y = S // X
    steps = sorted(
        ((i // X, i % X) for i in range(S)), key=lambda yx: ((yx[0] > 0) + (yx[1] > 0), yx)
    )
    near = [d for d in range(1, S) if 0 in steps[d]]
    far = [d for d in range(1, S) if 0 not in steps[d]]

    def sp_place(d, way=1):
        dy, dx = steps[d]
        y = lax.rem(lax.div(me, X) + (dy if way > 0 else Y - dy), Y)
        x = lax.rem(lax.rem(me, X) + (dx if way > 0 else X - dx), X)
        return y * X + x

    def sp_peer(d, way=1):
        return {"sp": sp_place(d, way), "tp": t}

    def z_peer(d):
        return {"sp": me, "tp": lax.rem(z + d, Z) * CORES + c}

    sends = []

    def put(src, dst, lane, slot, who):
        copy = pltpu.make_async_remote_copy(
            src_ref=src, dst_ref=dst, send_sem=send.at[lane, slot], recv_sem=recv.at[lane, slot],
            device_id=who, device_id_type=MESH,
        )
        copy.start()
        sends.append(copy)
        return copy

    mine = pl.ds(pl.multiple_of(c * half, half), half)
    others = pl.ds(pl.multiple_of((1 - c) * half, half), half)
    pairs = (
        (source_h.at[mine], source.at[mine]), (wk_h, wkv.at[:, :HEAD]), (wv_h, wkv.at[:, HEAD:]),
        (target_h, target), (wq_h, wq), (cot_h, cot), (wo_h, wo),
        (sgain_h, sgain), (tgain_h, tgain), (source_h.at[others], source.at[others]),
    )
    loads = [pltpu.make_async_copy(a, b, load_sem.at[i]) for i, (a, b) in enumerate(pairs)]
    for i in (7, 0, 1, 2):
        loads[i].start()

    barrier = pltpu.get_barrier_semaphore()
    friends = [sibling] + [sp_peer(d) for d in range(1, S)] + [z_peer(d) for d in range(1, Z)]
    for who in friends:
        pl.semaphore_signal(barrier, inc=1, device_id=who, device_id_type=MESH)

    loads[7].wait()
    loads[0].wait()
    for i in (9, 3, 5, 8, 4, 6):
        loads[i].start()
    norm_into(source, sgain, normed, 32, c * half, half)
    loads[1].wait()
    loads[2].wait()
    kv[0, c] = dot(normed[mine, :], wkv[...]).astype(BF16)
    pl.semaphore_wait(barrier, len(friends))
    kv_put = [None] + [put(kv.at[0, c], kv.at[d, c], 0, d, sp_peer(d)) for d in range(1, S)]
    loads[5].wait()
    cot_put = [None]
    for d in range(1, S):
        columns = pl.ds(pl.multiple_of(sp_place(d) * W, 128), W)
        rows = pl.ds(pl.multiple_of(c * thalf, thalf), thalf)
        cot_put.append(put(cot.at[rows, columns], cotb.at[d, c], 1, d, sp_peer(d)))

    loads[9].wait()
    norm_into(source, sgain, normed, 32, (1 - c) * half, half)
    kv[0, 1 - c] = dot(normed[others, :], wkv[...]).astype(BF16)
    loads[8].wait()
    loads[3].wait()
    norm_into(target, tgain, normed, 32, 0, TR)
    loads[4].wait()
    query = dot(normed[:TR, :], wq[...]).astype(BF16)
    loads[6].wait()
    grad = dot(cot[...], wo[...], NT).astype(BF16)
    q_rows = jnp.concatenate([query[:, h * HEAD:(h + 1) * HEAD] for h in range(H)], axis=0)
    g_rows = jnp.concatenate([grad[:, h * HEAD:(h + 1) * HEAD] for h in range(H)], axis=0)

    def pair(d):
        both = jnp.concatenate([kv[d,0],kv[d,1]],axis=0)
        return both[:, :HEAD], both[:, HEAD:]

    def exponents(d):
        k, v = pair(d)
        e = jnp.exp2(dot(k, q_rows, NT) * (inv_root * math.log2(math.e)))
        e_buf[d] = e
        return jnp.sum(e, axis=0, keepdims=True), dot(v, e.astype(BF16), TN)

    total, out_t = exponents(0)
    kv_fwd = [None]
    for d in range(1, S):
        kv_put[d].wait_recv()
        kv_fwd.append(put(kv.at[d, c], kv.at[d, c], 2, d, sibling))
    for d in range(1, S):
        kv_fwd[d].wait_recv()
        more, out_more = exponents(d)
        total, out_t = total + more, out_t + out_more
    inv_total = 1.0 / total
    att_t = (out_t * inv_total).astype(BF16)
    att[0] = att_t
    delta = jnp.sum(att_t.astype(F32) * g_rows.astype(F32).T, axis=0, keepdims=True)
    att_put = {d: put(att.at[0], att.at[d], 3, d, sp_peer(d)) for d in near}

    def spread(d, grads):
        if SR % 8:
            stage[...] = grads
        for place in range(T):
            rows = slice(place * SR, (place + 1) * SR)
            block = stage[rows, :] if SR % 8 else grads[rows]
            kvg[place % CORES, d, place // CORES] = block.astype(BF16)

    def settle(d):
        kvg_put[d].wait_recv()
        red[d] = (kvg[c, d].astype(F32) + kvg_in[d].astype(F32)).astype(BF16)
        if d:
            return put(red.at[d], red_in.at[d], 5, d, sp_peer(d, -1))

    kvg_put = {}
    red_put = {}
    gq_t = None
    order = list(range(S - 1, -1, -1))
    for step, d in enumerate(order):
        k, v = pair(d)
        p = e_buf[d] * inv_total
        score_grad = (p * (dot(v, g_rows, NT) - delta)).astype(BF16)
        part = dot(k, score_grad, TN)
        gq_t = part if gq_t is None else gq_t + part
        k_grad = dot(score_grad, q_rows) * inv_root
        v_grad = dot(p.astype(BF16), g_rows)
        spread(d, jnp.concatenate([k_grad, v_grad], axis=1))
        kvg_put[d] = put(kvg.at[1 - c, d], kvg_in.at[d], 4, d, sibling)
        if step:
            red_put[order[step - 1]] = settle(order[step - 1])

    for d in far:
        att_put[d] = put(att.at[0], att.at[d], 3, d, sp_peer(d))
    gq_t = gq_t * inv_root
    gq = jnp.concatenate([gq_t[:, h * TR:(h + 1) * TR].T for h in range(H)], axis=1).astype(BF16)
    pulled = dot(gq, wq[...], NT)
    for place in range(T):
        if RR % 8:
            if place == 0:
                normed_rows = stage_rows(e_buf, pulled)
            block = normed_rows(place * RR, RR)
        else:
            block = pulled[place * RR:(place + 1) * RR]
        pt[place % CORES, place // CORES] = block.astype(BF16)
    pt_put = put(pt.at[1 - c], pt_in, 6, 0, sibling)
    settle(0)
    cot_fwd = [None]
    for d in range(1, S):
        cot_put[d].wait_recv()
        cot_fwd.append(put(cotb.at[d, c], cotb.at[d, c], 7, d, sibling))
    pt_put.wait_recv()
    ptr[...] = (pt[c].astype(F32) + pt_in[...].astype(F32)).astype(BF16)
    ptr_put = [None] + [
        put(ptr.at[lax.rem(z + d, Z)], ptr_in.at[d], 8, d, z_peer(d)) for d in range(1, Z)
    ]
    summed = red[0].astype(F32)
    for d in range(1, S):
        red_put[d].wait_recv()
        summed = summed + red_in[d].astype(F32)
    red2[...] = summed.astype(BF16)
    fin_put = [None] + [
        put(red2.at[lax.rem(z + d, Z)], fin_in.at[d], 9, d, z_peer(d)) for d in range(1, Z)
    ]

    att_all, cot_all = [att[0]], [cot[:, pl.ds(pl.multiple_of(me * W, 128), W)]]
    for d in range(1, S):
        att_put[d].wait_recv()
        cot_fwd[d].wait_recv()
        att_all.append(att[d])
        cot_all.append(jnp.concatenate([cotb[d,0],cotb[d,1]],axis=0))
    cot_rows = jnp.concatenate(cot_all, axis=0)
    for h in range(H):
        left = jnp.concatenate([a[:, h * TR:(h + 1) * TR] for a in att_all], axis=1)
        go_ref[h * HEAD:(h + 1) * HEAD, :] = dot(left, cot_rows).astype(BF16)

    writes = [
        pltpu.make_async_copy(a, b, load_sem.at[i])
        for i, (a, b) in enumerate(((go_ref, go_out), (gt_ref, gt_out), (gs_ref, gs_out)))
    ]
    writes[0].start()
    up = ptr[z].astype(F32)
    for d in range(1, Z):
        ptr_put[d].wait_recv()
        up = up + ptr_in[d].astype(F32)
    gt_ref[...] = norm_back(own_rows(target, t, RR), tgain[...], up).astype(BF16)
    writes[1].start()
    last = red2[z].astype(F32)
    for d in range(1, Z):
        fin_put[d].wait_recv()
        last = last + fin_in[d].astype(F32)
    up = dot(last.astype(BF16), wkv[...], NT)
    gs_ref[...] = norm_back(own_rows(source, t, SR), sgain[...], up).astype(BF16)
    writes[2].start()
    for copy in sends:
        copy.wait_send()
    for copy in writes:
        copy.wait()


def stage_rows(buf, rows):
    width = buf.shape[2]
    bands = rows.shape[1] // width
    for i in range(bands):
        buf[i, :rows.shape[0], :] = rows[:, i * width:(i + 1) * width]
    return lambda start, count: jnp.concatenate(
        [buf[i, start:start + count, :] for i in range(bands)], axis=1
    )


def on_device(S, T, target, source, cotangent, target_gain, source_gain, w_query, w_key, w_value, w_out):
    TR, D = target.shape
    SG = source.shape[0]
    QW = w_query.shape[1]
    R = QW // HEAD * TR
    Z = T // CORES
    SR, RR, W = SG // T, TR // T, D // S
    N = max(S, Z)
    hbm = pl.BlockSpec(memory_space=pltpu.HBM)
    V = pltpu.VMEM
    results = pl.pallas_call(
        functools.partial(kernel, S, T),
        out_shape=(
            jax.ShapeDtypeStruct((RR, D), BF16),
            jax.ShapeDtypeStruct((SR, D), BF16),
            jax.ShapeDtypeStruct((QW, W), BF16),
        ),
        in_specs=[hbm] * 9,
        out_specs=(hbm, hbm, hbm),
        scratch_shapes=[
            V((TR, D), BF16), V((SG, D), BF16), V((TR, D), BF16), V((1, D), F32), V((1, D), F32),
            V((D, QW), BF16), V((D, 2 * HEAD), BF16), V((QW, D), BF16),
            V((max(SG, TR), D), BF16),
            V((S, 2, SG // 2, 2 * HEAD), BF16), V((S, 2, TR // 2, W), BF16),
            V((S, HEAD, R), BF16), V((S, SG, R), F32),
            V((CORES, S, Z, SR, 2 * HEAD), BF16), V((S, Z, SR, 2 * HEAD), BF16),
            V((S, Z, SR, 2 * HEAD), BF16), V((S, Z, SR, 2 * HEAD), BF16),
            V((Z, SR, 2 * HEAD), BF16), V((Z, SR, 2 * HEAD), BF16),
            V((CORES, Z, RR, D), BF16), V((Z, RR, D), BF16), V((Z, RR, D), BF16), V((Z, RR, D), BF16),
            V((SG, 2 * HEAD), F32),
            V((RR, D), BF16), V((SR, D), BF16), V((QW, W), BF16),
            pltpu.SemaphoreType.DMA((10,)),
            pltpu.SemaphoreType.DMA((10, N)),
            pltpu.SemaphoreType.DMA((10, N)),
        ],
        compiler_params=pltpu.CompilerParams(
            collective_id=0, has_side_effects=True, vmem_limit_bytes=60 * 1024 * 1024
        ),
        name="attn_back",
    )(
        target, source, cotangent, target_gain.reshape(1, D), source_gain.reshape(1, D),
        w_query, w_key, w_value, w_out,
    )
    return pl.pallas_call(
        put_out,
        out_shape=tuple(jax.ShapeDtypeStruct(r.shape, r.dtype) for r in results),
        in_specs=[hbm, hbm, hbm],
        out_specs=(hbm, hbm, hbm),
        scratch_shapes=[V(r.shape, r.dtype) for r in results]
        + [pltpu.SemaphoreType.DMA((3,)), pltpu.SemaphoreType.DMA((3,))],
        compiler_params=pltpu.CompilerParams(vmem_limit_bytes=60 * 1024 * 1024),
        name="put_out",
    )(*results)


def put_out(a, b, c, a_out, b_out, c_out, a_mid, b_mid, c_mid, in_sem, out_sem):
    trios = ((a, a_mid, a_out), (b, b_mid, b_out), (c, c_mid, c_out))
    ins = [pltpu.make_async_copy(x, y, in_sem.at[i]) for i, (x, y, _) in enumerate(trios)]
    outs = [pltpu.make_async_copy(x, y, out_sem.at[i]) for i, (_, x, y) in enumerate(trios)]
    for copy in ins:
        copy.start()
    for before, after in zip(ins, outs):
        before.wait()
        after.start()
    for copy in outs:
        copy.wait()


def solution(mesh):
    in_specs = (
        P("sp", None), P("sp", None), P("sp", None), P(), P(),
        P(None, "tp"), P(), P(), P("tp", None),
    )
    out_specs = (P(("sp", "tp"), None), P(("sp", "tp"), None), P("tp", "sp"))
    return jax.shard_map(
        functools.partial(on_device, mesh.shape["sp"], mesh.shape["tp"]),
        mesh=mesh, in_specs=in_specs, out_specs=out_specs, check_vma=False,
    )
```

```python
import functools
import math

import jax
import jax.numpy as jnp
from jax import lax
from jax.experimental import pallas as pl
from jax.experimental.pallas import tpu as pltpu
from jax.sharding import PartitionSpec as P

HEAD = 128
NORM_EPS = 1e-06
CORES = 2
F32 = jnp.float32
BF16 = jnp.bfloat16
MESH = pl.DeviceIdType.MESH
NN = (((1,), (0,)), ((), ()))
NT = (((1,), (1,)), ((), ()))
TN = (((0,), (0,)), ((), ()))


def dot(a, b, dims=NN):
    return lax.dot_general(a, b, dims, preferred_element_type=F32)


def inv_rms_of(wide):
    return lax.rsqrt(jnp.mean(wide * wide, axis=1, keepdims=True) + NORM_EPS)


def norm_into(src, gain, dst, block, base, count):
    def body(i, _):
        rows = pl.ds(pl.multiple_of(base + i * block, block), block)
        wide = src[rows, :].astype(F32)
        dst[rows, :] = (wide * inv_rms_of(wide) * gain[...]).astype(BF16)
        return 0

    lax.fori_loop(0, count // block, body, 0)


def unit_rows_of(wide):
    inv = inv_rms_of(wide)
    return inv, wide * inv


def norm_back(inv, unit, gain, upstream):
    pulled = upstream * gain
    return inv * (pulled - unit * jnp.mean(pulled * unit, axis=1, keepdims=True))


def own_rows(ref, place, rows):
    if rows % 16 == 0:
        return ref[pl.ds(pl.multiple_of(place * rows, 16), rows), :].astype(F32)
    padded = -(-rows // 16) * 16
    line = lax.broadcasted_iota(jnp.int32, (padded, ref.shape[0]), 0) + place * rows
    column = lax.broadcasted_iota(jnp.int32, (padded, ref.shape[0]), 1)
    pick = jnp.where(line == column, 1.0, 0.0).astype(BF16)
    return dot(pick, ref[...])[:rows]


def kernel(
    S, T,
    target_h, source_h, cot_h, tgain_h, sgain_h, wq_h, wk_h, wv_h, wo_h,
    gt_out, gs_out, go_out,
    target, source, cot, tgain, sgain, wq, wkv, wo, normed, kv, cotb, att, e_buf, pg_buf,
    kvg, kvg_in, red, red_in, red2, fin_in, pt, pt_in, ptr, ptr_in, stage,
    gt_ref, gs_ref, go_ref, load_sem, send, recv,
):
    Z = T // CORES
    me, t = lax.axis_index("sp"), lax.axis_index("tp")
    c, z = lax.rem(t, CORES), lax.div(t, CORES)
    sibling = {"sp": me, "tp": z * CORES + (1 - c)}
    TR, D = target.shape
    SG = source.shape[0]
    QW = wq.shape[1]
    H = QW // HEAD
    half = SG // 2
    thalf = TR // 2
    W = D // S
    SR, RR = SG // T, TR // T
    inv_root = HEAD ** (-0.5)

    X = math.isqrt(S) if math.isqrt(S) ** 2 == S else S
    Y = S // X
    steps = sorted(
        ((i // X, i % X) for i in range(S)), key=lambda yx: ((yx[0] > 0) + (yx[1] > 0), yx)
    )
    near = [d for d in range(1, S) if 0 in steps[d]]
    far = [d for d in range(1, S) if 0 not in steps[d]]

    def sp_place(d, way=1):
        dy, dx = steps[d]
        y = lax.rem(lax.div(me, X) + (dy if way > 0 else Y - dy), Y)
        x = lax.rem(lax.rem(me, X) + (dx if way > 0 else X - dx), X)
        return y * X + x

    def sp_peer(d, way=1):
        return {"sp": sp_place(d, way), "tp": t}

    def z_peer(d):
        return {"sp": me, "tp": lax.rem(z + d, Z) * CORES + c}

    sends = []

    def put(src, dst, lane, slot, who):
        copy = pltpu.make_async_remote_copy(
            src_ref=src, dst_ref=dst, send_sem=send.at[lane, slot], recv_sem=recv.at[lane, slot],
            device_id=who, device_id_type=MESH,
        )
        copy.start()
        sends.append(copy)
        return copy

    mine = pl.ds(pl.multiple_of(c * half, half), half)
    others = pl.ds(pl.multiple_of((1 - c) * half, half), half)
    pairs = (
        (source_h.at[mine], source.at[mine]), (wk_h, wkv.at[:, :HEAD]), (wv_h, wkv.at[:, HEAD:]),
        (target_h, target), (wq_h, wq), (cot_h, cot), (wo_h, wo),
        (sgain_h, sgain), (tgain_h, tgain), (source_h.at[others], source.at[others]),
    )
    loads = [pltpu.make_async_copy(a, b, load_sem.at[i]) for i, (a, b) in enumerate(pairs)]
    for i in (7, 0, 1, 2):
        loads[i].start()

    barrier = pltpu.get_barrier_semaphore()
    friends = [sibling] + [sp_peer(d) for d in range(1, S)] + [z_peer(d) for d in range(1, Z)]
    for who in friends:
        pl.semaphore_signal(barrier, inc=1, device_id=who, device_id_type=MESH)

    loads[7].wait()
    loads[0].wait()
    for i in (9, 3, 5, 8, 4, 6):
        loads[i].start()
    norm_into(source, sgain, normed, 32, c * half, half)
    loads[1].wait()
    loads[2].wait()
    kv[0, c] = dot(normed[mine, :], wkv[...]).astype(BF16)
    pl.semaphore_wait(barrier, len(friends))
    kv_put = {d: put(kv.at[0, c], kv.at[d, c], 0, d, sp_peer(d)) for d in far + near}
    loads[5].wait()
    cot_put = [None]
    for d in range(1, S):
        columns = pl.ds(pl.multiple_of(sp_place(d) * W, 128), W)
        rows = pl.ds(pl.multiple_of(c * thalf, thalf), thalf)
        cot_put.append(put(cot.at[rows, columns], cotb.at[d, c], 1, d, sp_peer(d)))

    loads[9].wait()
    norm_into(source, sgain, normed, 32, (1 - c) * half, half)
    kv[0, 1 - c] = dot(normed[others, :], wkv[...]).astype(BF16)
    loads[8].wait()
    loads[3].wait()
    norm_into(target, tgain, normed, 32, 0, TR)
    loads[4].wait()
    query = dot(normed[:TR, :], wq[...]).astype(BF16)
    loads[6].wait()
    grad = dot(cot[...], wo[...], NT).astype(BF16)
    q_rows = jnp.concatenate([query[:, h * HEAD:(h + 1) * HEAD] for h in range(H)], axis=0)
    g_rows = jnp.concatenate([grad[:, h * HEAD:(h + 1) * HEAD] for h in range(H)], axis=0)

    def pair(d):
        both = jnp.concatenate([kv[d,0],kv[d,1]],axis=0)
        return both[:, :HEAD], both[:, HEAD:]

    def exponents(d):
        k, v = pair(d)
        e = jnp.exp2(dot(k, q_rows, NT) * (inv_root * math.log2(math.e)))
        e_buf[d] = e
        pg_buf[d] = dot(v, g_rows, NT)
        return jnp.sum(e, axis=0, keepdims=True), dot(v, e.astype(BF16), TN)

    total, out_t = exponents(0)
    kv_fwd = {}
    middle = len(near) // 2
    arrivals = near[middle:] + far + near[:middle]
    for step, d in enumerate(arrivals + [None]):
        if d is not None:
            kv_put[d].wait_recv()
            kv_fwd[d] = put(kv.at[d, c], kv.at[d, c], 2, d, sibling)
        if step:
            before = arrivals[step - 1]
            kv_fwd[before].wait_recv()
            more, out_more = exponents(before)
            total, out_t = total + more, out_t + out_more
    inv_total = 1.0 / total
    att_t = (out_t * inv_total).astype(BF16)
    att[0] = att_t
    delta = jnp.sum(att_t.astype(F32) * g_rows.astype(F32).T, axis=0, keepdims=True)
    att_put = {d: put(att.at[0], att.at[d], 3, d, sp_peer(d)) for d in near}

    def spread(d, grads):
        if SR % 8:
            stage[...] = grads
        for place in range(T):
            rows = slice(place * SR, (place + 1) * SR)
            block = stage[rows, :] if SR % 8 else grads[rows]
            kvg[place % CORES, d, place // CORES] = block.astype(BF16)

    def settle(d):
        kvg_put[d].wait_recv()
        red[d] = (kvg[c, d].astype(F32) + kvg_in[d].astype(F32)).astype(BF16)
        if d:
            return put(red.at[d], red_in.at[d], 5, d, sp_peer(d, -1))

    kvg_put = {}
    red_put = {}
    gq_t = None
    order = list(range(S - 1, -1, -1))
    for step, d in enumerate(order):
        k, _ = pair(d)
        p = e_buf[d] * inv_total
        score_grad = (p * (pg_buf[d] - delta)).astype(BF16)
        part = dot(k, score_grad, TN)
        gq_t = part if gq_t is None else gq_t + part
        k_grad = dot(score_grad, q_rows) * inv_root
        v_grad = dot(p.astype(BF16), g_rows)
        spread(d, jnp.concatenate([k_grad, v_grad], axis=1))
        kvg_put[d] = put(kvg.at[1 - c, d], kvg_in.at[d], 4, d, sibling)
        if step:
            red_put[order[step - 1]] = settle(order[step - 1])

    for d in far:
        att_put[d] = put(att.at[0], att.at[d], 3, d, sp_peer(d))
    gq_t = gq_t * inv_root
    gq = jnp.concatenate([gq_t[:, h * TR:(h + 1) * TR].T for h in range(H)], axis=1).astype(BF16)
    pulled = dot(gq, wq[...], NT)
    for place in range(T):
        if RR % 8:
            if place == 0:
                normed_rows = stage_rows(e_buf, pulled)
            block = normed_rows(place * RR, RR)
        else:
            block = pulled[place * RR:(place + 1) * RR]
        pt[place % CORES, place // CORES] = block.astype(BF16)
    pt_put = put(pt.at[1 - c], pt_in, 6, 0, sibling)
    settle(0)
    cot_fwd = [None]
    for d in range(1, S):
        cot_put[d].wait_recv()
        cot_fwd.append(put(cotb.at[d, c], cotb.at[d, c], 7, d, sibling))
    pt_put.wait_recv()
    ptr[...] = (pt[c].astype(F32) + pt_in[...].astype(F32)).astype(BF16)
    ptr_put = [None] + [
        put(ptr.at[lax.rem(z + d, Z)], ptr_in.at[d], 8, d, z_peer(d)) for d in range(1, Z)
    ]
    summed = red[0].astype(F32)
    for d in range(1, S):
        red_put[d].wait_recv()
        summed = summed + red_in[d].astype(F32)
    red2[...] = summed.astype(BF16)
    fin_put = [None] + [
        put(red2.at[lax.rem(z + d, Z)], fin_in.at[d], 9, d, z_peer(d)) for d in range(1, Z)
    ]

    att_all, cot_all = [att[0]], [cot[:, pl.ds(pl.multiple_of(me * W, 128), W)]]
    for d in range(1, S):
        att_put[d].wait_recv()
        cot_fwd[d].wait_recv()
        att_all.append(att[d])
        cot_all.append(jnp.concatenate([cotb[d,0],cotb[d,1]],axis=0))
    cot_rows = jnp.concatenate(cot_all, axis=0)
    for h in range(H):
        left = jnp.concatenate([a[:, h * TR:(h + 1) * TR] for a in att_all], axis=1)
        go_ref[h * HEAD:(h + 1) * HEAD, :] = dot(left, cot_rows).astype(BF16)

    writes = [
        pltpu.make_async_copy(a, b, load_sem.at[i])
        for i, (a, b) in enumerate(((go_ref, go_out), (gt_ref, gt_out), (gs_ref, gs_out)))
    ]
    writes[0].start()
    target_inv, target_unit = unit_rows_of(own_rows(target, t, RR))
    up = ptr[z].astype(F32)
    for d in range(1, Z):
        ptr_put[d].wait_recv()
        up = up + ptr_in[d].astype(F32)
    gt_ref[...] = norm_back(target_inv, target_unit, tgain[...], up).astype(BF16)
    writes[1].start()
    source_inv, source_unit = unit_rows_of(own_rows(source, t, SR))
    last = red2[z].astype(F32)
    for d in range(1, Z):
        fin_put[d].wait_recv()
        last = last + fin_in[d].astype(F32)
    up = dot(last.astype(BF16), wkv[...], NT)
    gs_ref[...] = norm_back(source_inv, source_unit, sgain[...], up).astype(BF16)
    writes[2].start()
    for copy in sends:
        copy.wait_send()
    for copy in writes:
        copy.wait()


def stage_rows(buf, rows):
    width = buf.shape[2]
    bands = rows.shape[1] // width
    for i in range(bands):
        buf[i, :rows.shape[0], :] = rows[:, i * width:(i + 1) * width]
    return lambda start, count: jnp.concatenate(
        [buf[i, start:start + count, :] for i in range(bands)], axis=1
    )


def on_device(S, T, target, source, cotangent, target_gain, source_gain, w_query, w_key, w_value, w_out):
    TR, D = target.shape
    SG = source.shape[0]
    QW = w_query.shape[1]
    R = QW // HEAD * TR
    Z = T // CORES
    SR, RR, W = SG // T, TR // T, D // S
    N = max(S, Z)
    hbm = pl.BlockSpec(memory_space=pltpu.HBM)
    V = pltpu.VMEM
    results = pl.pallas_call(
        functools.partial(kernel, S, T),
        out_shape=(
            jax.ShapeDtypeStruct((RR, D), BF16),
            jax.ShapeDtypeStruct((SR, D), BF16),
            jax.ShapeDtypeStruct((QW, W), BF16),
        ),
        in_specs=[hbm] * 9,
        out_specs=(hbm, hbm, hbm),
        scratch_shapes=[
            V((TR, D), BF16), V((SG, D), BF16), V((TR, D), BF16), V((1, D), F32), V((1, D), F32),
            V((D, QW), BF16), V((D, 2 * HEAD), BF16), V((QW, D), BF16),
            V((max(SG, TR), D), BF16),
            V((S, 2, SG // 2, 2 * HEAD), BF16), V((S, 2, TR // 2, W), BF16),
            V((S, HEAD, R), BF16), V((S, SG, R), F32), V((S, SG, R), F32),
            V((CORES, S, Z, SR, 2 * HEAD), BF16), V((S, Z, SR, 2 * HEAD), BF16),
            V((S, Z, SR, 2 * HEAD), BF16), V((S, Z, SR, 2 * HEAD), BF16),
            V((Z, SR, 2 * HEAD), BF16), V((Z, SR, 2 * HEAD), BF16),
            V((CORES, Z, RR, D), BF16), V((Z, RR, D), BF16), V((Z, RR, D), BF16), V((Z, RR, D), BF16),
            V((SG, 2 * HEAD), F32),
            V((RR, D), BF16), V((SR, D), BF16), V((QW, W), BF16),
            pltpu.SemaphoreType.DMA((10,)),
            pltpu.SemaphoreType.DMA((10, N)),
            pltpu.SemaphoreType.DMA((10, N)),
        ],
        compiler_params=pltpu.CompilerParams(
            collective_id=0, has_side_effects=True, vmem_limit_bytes=60 * 1024 * 1024
        ),
        name="attn_back",
    )(
        target, source, cotangent, target_gain.reshape(1, D), source_gain.reshape(1, D),
        w_query, w_key, w_value, w_out,
    )
    return pl.pallas_call(
        put_out,
        out_shape=tuple(jax.ShapeDtypeStruct(r.shape, r.dtype) for r in results),
        in_specs=[hbm, hbm, hbm],
        out_specs=(hbm, hbm, hbm),
        scratch_shapes=[V(r.shape, r.dtype) for r in results]
        + [pltpu.SemaphoreType.DMA((3,)), pltpu.SemaphoreType.DMA((3,))],
        compiler_params=pltpu.CompilerParams(vmem_limit_bytes=60 * 1024 * 1024),
        name="put_out",
    )(*results)


def put_out(a, b, c, a_out, b_out, c_out, a_mid, b_mid, c_mid, in_sem, out_sem):
    trios = ((a, a_mid, a_out), (b, b_mid, b_out), (c, c_mid, c_out))
    ins = [pltpu.make_async_copy(x, y, in_sem.at[i]) for i, (x, y, _) in enumerate(trios)]
    outs = [pltpu.make_async_copy(x, y, out_sem.at[i]) for i, (_, x, y) in enumerate(trios)]
    for copy in ins:
        copy.start()
    for before, after in zip(ins, outs):
        before.wait()
        after.start()
    for copy in outs:
        copy.wait()


def solution(mesh):
    in_specs = (
        P("sp", None), P("sp", None), P("sp", None), P(), P(),
        P(None, "tp"), P(), P(), P("tp", None),
    )
    out_specs = (P(("sp", "tp"), None), P(("sp", "tp"), None), P("tp", "sp"))
    return jax.shard_map(
        functools.partial(on_device, mesh.shape["sp"], mesh.shape["tp"]),
        mesh=mesh, in_specs=in_specs, out_specs=out_specs, check_vma=False,
    )
```
